32 devices in a mesh: ra: 8 (over z, y), cb: 4 (over x, core).
Axes of the slice: x: 2, y: 2, z: 4, core: 2. Of those that a mesh axis runs over, the one named last changes fastest.
Arguments:
- tokens: bfloat16 [2048, 4096], P('ra'), may hold values from -16 to 16
- norm_gain: float32 [2, 2048], replicated, may hold values from 0.1 to 1.9
- up_weight: float32 [2, 2048, 6144], P(None, 'ra', 'cb'), may hold values from -0.125 to 0.125
- gate_weight: float32 [2, 2048, 6144], P(None, 'ra', 'cb'), may hold values from -0.125 to 0.125
- up_scale: float32 [2, 6144], P(None, 'cb'), may hold values from 0.5 to 2
- gate_scale: float32 [2, 6144], P(None, 'cb'), may hold values from 0.5 to 2
- up_taps: float32 [2, 3, 6144], P(None, None, 'cb'), may hold values from -3 to 3
- gate_taps: float32 [2, 3, 6144], P(None, None, 'cb'), may hold values from -3 to 3
- down_weight: float32 [2, 2048, 6144], P(None, 'ra', 'cb'), may hold values from -0.078125 to 0.078125
- down_scale: float32 [2, 2048], replicated, may hold values from 0.5 to 2
Outputs:
- mixed: bfloat16 [2048, 4096], P('ra')
The draws below stay inside these ranges and needn't reach their ends.
All inputs are finite; a program needn't handle non-finite values.
Results may differ from the reference program's by a relative error of at most 0.024.
Values may be sent and summed in bfloat16 or wider, within the bound.
A program may use at most 128 MiB of HBM per device.

```python
import math
import jax
import jax.numpy as jnp
from jax import lax

D = 2048
FF = 6144
KW = 3
LAYERS = 2
TOKENS = 4096
N_RA = 8
N_CB = 4


def draw_tokens(key, part):
    first, second, third = jax.random.split(key, 3)
    blocks = jnp.exp(jax.random.uniform(second, (N_RA,), jnp.float32, math.log(0.3), math.log(3.0)))
    features = jnp.repeat(blocks, D // N_RA, total_repeat_length=D)
    base = jnp.clip(jax.random.normal(first, (D, TOKENS), jnp.float32), -4.0, 4.0)
    return (base * features[:, None]).astype(jnp.bfloat16)


def shard_levels(rng, extent, cuts, smallest, high):
    gain, own = 1.0, jax.random.fold_in(rng, 6)
    for position, parts in cuts:
        draws = jnp.exp(jax.random.uniform(jax.random.fold_in(own, position), (parts,), jnp.float32, smallest / len(cuts), high / len(cuts)))
        gain = gain * jnp.repeat(draws, extent[position] // parts).reshape([-1 if axis == position else 1 for axis in range(len(extent))])
    return gain


def normal_values(stream_key, extent, scale, bound, pieces=(), dtype=jnp.bfloat16):
    level = shard_levels(stream_key, extent, pieces, -0.22, 0.18) if pieces else 1.0
    values = jax.random.normal(stream_key, extent, jnp.float32) * scale * level
    return jnp.minimum(jnp.maximum(values, -bound), bound).astype(dtype)


def setup_inputs(seed: int = 0) -> dict:
    splits = jax.random.split(jax.random.key(seed), 11)
    return {
        "tokens": draw_tokens(jax.random.fold_in(splits[10], 71), 0),
        "norm_gain": jnp.clip(1.0 + 0.18 * jax.random.normal(splits[1], (LAYERS, D), jnp.float32), 0.1, 1.9),
        "up_weight": normal_values(splits[2], (LAYERS, D, FF), D ** -0.5, 0.125, ((1, 8), (2, 4)), jnp.float32),
        "gate_weight": normal_values(splits[3], (LAYERS, D, FF), D ** -0.5, 0.125, ((1, 8), (2, 4)), jnp.float32),
        "up_scale": jnp.clip(jnp.exp(math.log(2.0) - 1.3862944 * jax.random.uniform(splits[4], (LAYERS, FF), jnp.float32) ** shard_levels(splits[4], (LAYERS, FF), ((1, 4),), -0.2, 0.2)), 0.5, 2.0),
        "gate_scale": jnp.clip(jnp.exp(math.log(2.0) - 1.3862944 * jax.random.uniform(splits[5], (LAYERS, FF), jnp.float32) ** shard_levels(splits[5], (LAYERS, FF), ((1, 4),), -0.2, 0.2)), 0.5, 2.0),
        "up_taps": normal_values(splits[6], (LAYERS, KW, FF), 0.6, 3.0, ((2, 4),), jnp.float32),
        "gate_taps": normal_values(splits[7], (LAYERS, KW, FF), 0.6, 3.0, ((2, 4),), jnp.float32),
        "down_weight": normal_values(splits[8], (LAYERS, D, FF), FF ** -0.5, 0.078125, ((1, 8), (2, 4)), jnp.float32),
        "down_scale": jnp.clip(jnp.exp(jax.random.uniform(splits[9], (LAYERS, D), jnp.float32, math.log(0.5), math.log(2.0))), 0.5, 2.0),
    }


EPS = 1e-06
RESIDUAL = 0.5

def causal_taps(values, taps):
    width = taps.shape[0]
    length = values.shape[0]
    padded = jnp.pad(values, ((width - 1, 0), (0, 0)))
    total = jnp.zeros_like(values)
    for k in range(width):
        total = total + taps[k][None, :] * padded[k:k + length]
    return total

def reference(tokens, norm_gain, up_weight, gate_weight, up_scale, gate_scale, up_taps, gate_taps, down_weight, down_scale):
    state = tokens.T
    block = FF // N_CB
    for layer in range(LAYERS):
        state_f = state.astype(jnp.float32)
        inverse = lax.rsqrt(lax.optimization_barrier(jnp.mean(state_f * state_f, axis=1, keepdims=True)) + EPS)
        scaled = (state_f * norm_gain[layer][None, :]).astype(jnp.bfloat16)
        up_raw = jnp.dot(scaled, up_weight[layer].astype(jnp.bfloat16), preferred_element_type=jnp.float32)
        gate_raw = jnp.dot(scaled, gate_weight[layer].astype(jnp.bfloat16), preferred_element_type=jnp.float32)
        up_pre = up_raw * inverse * up_scale[layer][None, :]
        gate_pre = gate_raw * inverse * gate_scale[layer][None, :]
        conv_up = causal_taps(up_pre, up_taps[layer])
        conv_gate = causal_taps(gate_pre, gate_taps[layer])
        hidden = (jax.nn.silu(conv_gate) * conv_up).astype(jnp.bfloat16)
        weight_b = down_weight[layer].astype(jnp.bfloat16)
        down = jnp.zeros((hidden.shape[0], weight_b.shape[0]), jnp.float32)
        for group in range(N_CB):
            term = jnp.dot(hidden[:, group * block:(group + 1) * block], weight_b[:, group * block:(group + 1) * block].T, preferred_element_type=jnp.float32)
            rounded = lax.optimization_barrier(term.astype(jnp.bfloat16))
            down = down + rounded.astype(jnp.float32)
        state = (down * down_scale[layer][None, :] + RESIDUAL * state_f).astype(jnp.bfloat16)
    return state.T
```

```python
import jax
import jax.numpy as jnp
from jax import lax
from jax.sharding import PartitionSpec as P


EPS = 1e-06
RESIDUAL = 0.5


def swap(value, axis, bit):
    count = lax.axis_size(axis)
    return lax.ppermute(value, axis, [(source, source ^ bit) for source in range(count)])


def doublings(low, high):
    bits = []
    while low < high:
        bits.append(low)
        low *= 2
    return bits


def valid_taps(values, taps):
    width = taps.shape[0]
    length = values.shape[0] - width + 1
    total = taps[0][None, :] * values[0:length]
    for k in range(1, width):
        total = total + taps[k][None, :] * values[k : k + length]
    return total


def per_device(
    tokens,
    norm_gain,
    up_weight,
    gate_weight,
    up_scale,
    gate_scale,
    up_taps,
    gate_taps,
    down_weight,
    down_scale,
):
    n_ra, n_cb = lax.axis_size("ra"), lax.axis_size("cb")
    n_y = 1 << ((n_ra.bit_length() - 1) // 2)
    r, j = lax.axis_index("ra"), lax.axis_index("cb")
    layers, rows, columns = up_weight.shape
    half = columns // 2
    members = 2 * n_cb
    groups = n_ra // 2
    length = tokens.shape[1]
    group_tokens = length // groups
    own_tokens = group_tokens // members
    member = (r // n_y) % 2

    steps = [("cb", bit, (j // bit) % 2) for bit in doublings(1, n_cb)] + [("ra", n_y, member)]

    far_bits = doublings(2 * n_y, n_ra) + doublings(1, n_y)
    chunk_offsets = [0]
    for bit in far_bits:
        chunk_offsets += [offset ^ bit for offset in chunk_offsets]
    order = [offset ^ low for offset in chunk_offsets for low in (0, n_y)]
    order_ids = jnp.array(order, jnp.int32) ^ r

    def first_token(device):
        z, y = device // n_y, device % n_y
        group = (z // 2) * n_y + y
        sub = 0
        for axis, bit, mine in steps:
            sub = sub * 2 + (mine if axis == "cb" else z % 2)
        return group * group_tokens + sub * own_tokens

    def collect(weight):
        weight = weight.astype(jnp.bfloat16)
        keep = lax.dynamic_slice_in_dim(weight, member * half, half, 1)
        give = lax.dynamic_slice_in_dim(weight, (1 - member) * half, half, 1)
        chunks = [jnp.concatenate([keep, swap(give, "ra", n_y)], axis=0)]
        for bit in far_bits:
            chunks = chunks + [swap(chunk, "ra", bit) for chunk in chunks]
        return chunks

    def other_order(value):
        parts = jnp.split(value, n_ra, axis=1)
        return jnp.concatenate([parts[k ^ 1] for k in range(n_ra)], axis=1)

    def mine_of(vector):
        return lax.dynamic_slice_in_dim(vector, member * half, half, vector.ndim - 1)

    def by_order(vector):
        return vector.reshape(n_ra, rows)[order_ids].reshape(-1)

    def along_group(value):
        for axis, bit, mine in reversed(steps):
            arrived = swap(value, axis, bit)
            if axis == "ra":
                arrived = other_order(arrived)
            value = jnp.where(
                mine == 0,
                jnp.concatenate([value, arrived], axis=0),
                jnp.concatenate([arrived, value], axis=0),
            )
        return value

    def sum_over_group(value):
        for axis, bit, mine in steps:
            count = value.shape[0] // 2
            keep = lax.dynamic_slice_in_dim(value, mine * count, count, 0)
            give = lax.dynamic_slice_in_dim(value, (1 - mine) * count, count, 0)
            arrived = swap(give.astype(jnp.bfloat16), axis, bit)
            if axis == "ra":
                arrived = other_order(arrived)
            value = keep + arrived.astype(jnp.float32)
        return value

    def from_previous(value):
        pairs = []
        for source in range(n_ra):
            z, y = source // n_y, source % n_y
            group = (z // 2) * n_y + y + 1
            if group < groups:
                pairs.append((source, ((group // n_y) * 2 + z % 2) * n_y + group % n_y))
        return lax.ppermute(value, "ra", pairs)

    pieces = []
    for offset in order:
        piece = lax.dynamic_slice_in_dim(tokens, first_token(r ^ offset), own_tokens, 1)
        pieces.append(swap(piece, "ra", offset) if offset else piece)
    state = jnp.concatenate(pieces, axis=0).T
    weights = [
        [collect(weight[layer]) for weight in (up_weight, gate_weight, down_weight)]
        for layer in range(layers)
    ]
    edge = up_taps.shape[1] - 1
    span = 2 * rows
    for layer in range(layers):
        up, gate, down = weights[layer]
        group_state = along_group(state).astype(jnp.float32)
        inverse = lax.rsqrt(jnp.mean(group_state * group_state, axis=1, keepdims=True) + EPS)
        scaled = (group_state * by_order(norm_gain[layer])[None, :]).astype(jnp.bfloat16)

        def product(chunks):
            total = None
            for k, chunk in enumerate(chunks):
                term = jnp.dot(
                    scaled[:, k * span : (k + 1) * span],
                    chunk,
                    preferred_element_type=jnp.float32,
                )
                total = term if total is None else total + term
            return total

        up_pre = product(up) * inverse * mine_of(up_scale[layer])[None, :]
        gate_pre = product(gate) * inverse * mine_of(gate_scale[layer])[None, :]
        tail = jnp.concatenate([up_pre[-edge:], gate_pre[-edge:]], axis=1)
        before = from_previous(tail)
        conv_up = valid_taps(
            jnp.concatenate([before[:, :half], up_pre], axis=0), mine_of(up_taps[layer])
        )
        conv_gate = valid_taps(
            jnp.concatenate([before[:, half:], gate_pre], axis=0), mine_of(gate_taps[layer])
        )
        hidden = (jax.nn.silu(conv_gate) * conv_up).astype(jnp.bfloat16)
        partial = jnp.concatenate(
            [
                lax.dot_general(
                    hidden,
                    chunk,
                    (((1,), (1,)), ((), ())),
                    preferred_element_type=jnp.float32,
                )
                for chunk in down
            ],
            axis=1,
        )
        total = sum_over_group(partial)
        state = (
            total * by_order(down_scale[layer])[None, :] + RESIDUAL * state.astype(jnp.float32)
        ).astype(jnp.bfloat16)

    turned = state.T.reshape(n_ra, rows, own_tokens)
    pieces = [
        swap(turned[k], "ra", offset) if offset else turned[k] for k, offset in enumerate(order)
    ]
    place = [order.index(k) for k in range(n_ra)]
    stacked = jnp.stack([pieces[k] for k in place])[jnp.arange(n_ra, dtype=jnp.int32) ^ r][None]
    for bit in reversed(doublings(1, n_cb)):
        arrived = swap(stacked, "cb", bit)
        stacked = jnp.where(
            (j // bit) % 2 == 0,
            jnp.concatenate([stacked, arrived], axis=0),
            jnp.concatenate([arrived, stacked], axis=0),
        )
    bits = len(doublings(1, n_cb))
    full = stacked.reshape((2,) * bits + (groups // n_y, 2, n_y, rows, own_tokens))
    axes = (bits + 3, bits, bits + 2) + tuple(range(bits)) + (bits + 1, bits + 4)
    return full.transpose(axes).reshape(rows, length)


def solution(mesh):
    placed = (
        P("ra", None),
        P(),
        P(None, "ra", "cb"),
        P(None, "ra", "cb"),
        P(None, "cb"),
        P(None, "cb"),
        P(None, None, "cb"),
        P(None, None, "cb"),
        P(None, "ra", "cb"),
        P(),
    )

    return jax.shard_map(
        per_device, mesh=mesh, in_specs=placed, out_specs=P("ra", None), check_vma=False
    )
```
